32 devices in a mesh: sp: 4 (over z), dp: 8 (over y, x, core).
Axes of the slice: x: 2, y: 2, z: 4, core: 2. Of those that a mesh axis runs over, the one named last changes fastest.
Arguments:
- tokens: bfloat16 [8, 768, 2048], P('dp', 'sp'), may hold values from -36 to 36
- query_weight: bfloat16 [2048, 2048], P('dp'), may hold values from -0.125 to 0.125
- key_weight: bfloat16 [2048, 512], P('dp'), may hold values from -0.125 to 0.125
- value_weight: bfloat16 [2048, 512], P('dp'), may hold values from -0.125 to 0.125
- forget_weight: bfloat16 [2048, 16], replicated, may hold values from -0.125 to 0.125
- forget_bias: float32 [16], replicated, may hold values from 3.4 to 9
Outputs:
- mixed: bfloat16 [8, 768, 2048], P('dp', 'sp')
The draws below stay inside these ranges and needn't reach their ends.
All inputs are finite; a program needn't handle non-finite values.
Results may differ from the reference program's by a relative error of at most 0.012.
Values may be sent and summed in bfloat16 or wider, within the bound.
A program may use at most 64 MiB of HBM per device.

```python
import math
import jax
import jax.numpy as jnp
from jax import lax

D = 2048
H = 16
DH = 128
KV = 4
SEQ = 768
NSEQ = 8


def draw_tokens(key, part):
    base_values = jnp.clip(jax.random.normal(key, (NSEQ, SEQ, D), jnp.float32), -4.0, 4.0)
    return base_values.astype(jnp.bfloat16)


def draw_forget_bias(key, part):
    fast_share = 0.5
    fast_heads = jax.random.uniform(jax.random.fold_in(key, 3), (H,)) < fast_share
    jitter = jax.random.uniform(jax.random.fold_in(key, 5), (H,), jnp.float32)
    return jnp.where(fast_heads, 3.4 + 0.8 * jitter, math.log(SEQ) + 0.4 * jitter).astype(jnp.float32)


def shard_levels(rng, extent, pieces, low, high):
    loudness, own = 1.0, jax.random.fold_in(rng, 6)
    for position, blocks in pieces:
        steps = jnp.exp(jax.random.uniform(jax.random.fold_in(own, position), (blocks,), jnp.float32, low / len(pieces), high / len(pieces)))
        loudness = loudness * jnp.repeat(steps, extent[position] // blocks).reshape([-1 if axis == position else 1 for axis in range(len(extent))])
    return loudness


def centred(key, extent, deviation, reach, shards=(), kind=jnp.bfloat16):
    drawn = deviation * jax.random.normal(key, extent, jnp.float32)
    if shards:
        drawn = drawn * shard_levels(key, extent, shards, -0.22, 0.18)
    return jnp.clip(drawn, -reach, reach).astype(kind)


def setup_inputs(seed: int = 0) -> dict:
    key_list = jax.random.split(jax.random.key(seed), 7)
    return {
        "tokens": draw_tokens(jax.random.fold_in(key_list[6], 71), 0),
        "query_weight": centred(key_list[1], (D, H * DH), D ** -0.5, 0.125, ((0, 8),)),
        "key_weight": centred(key_list[2], (D, KV * DH), D ** -0.5, 0.125, ((0, 8),)),
        "value_weight": centred(key_list[3], (D, KV * DH), D ** -0.5, 0.125, ((0, 8),)),
        "forget_weight": centred(key_list[4], (D, H), D ** -0.5, 0.125),
        "forget_bias": draw_forget_bias(jax.random.fold_in(key_list[6], 71), 0),
    }


def pick_block(length):
    for candidate in (512, 384, 256, 128):
        if length % candidate == 0:
            return candidate
    return length


def reference(tokens, query_weight, key_weight, value_weight, forget_weight, forget_bias):
    seq_count, seq_length, model_width = tokens.shape
    head_count = forget_weight.shape[1]
    head_dim = query_weight.shape[1] // head_count
    key_heads = key_weight.shape[1] // head_dim
    group_size = head_count // key_heads
    token_rows = tokens.reshape(seq_count * seq_length, model_width)
    query_rows = jnp.dot(token_rows, query_weight, preferred_element_type=jnp.float32).astype(jnp.bfloat16)
    query_rows = query_rows.reshape(seq_count, seq_length, head_count, head_dim)
    key_rows = jnp.dot(token_rows, key_weight, preferred_element_type=jnp.float32).astype(jnp.bfloat16)
    key_rows = key_rows.reshape(seq_count, seq_length, key_heads, head_dim)
    value_rows = jnp.dot(token_rows, value_weight, preferred_element_type=jnp.float32).astype(jnp.bfloat16)
    value_rows = value_rows.reshape(seq_count, seq_length, key_heads, head_dim)
    gate_input = jnp.dot(token_rows, forget_weight, preferred_element_type=jnp.float32) + forget_bias[None, :]
    log_gate = jax.nn.log_sigmoid(gate_input).astype(jnp.bfloat16).reshape(seq_count, seq_length, head_count)
    decay_sum = jnp.cumsum(log_gate.astype(jnp.float32), axis=1)
    block_size = pick_block(seq_length)
    block_count = seq_length // block_size
    score_scale = head_dim ** -0.5
    positions = jnp.arange(seq_length, dtype=jnp.int32)
    offsets = jnp.arange(block_size, dtype=jnp.int32)

    def one_block(flat_index):
        seq_index = flat_index // (head_count * block_count)
        head_index = (flat_index // block_count) % head_count
        block_index = flat_index % block_count
        first_row = block_index * block_size
        zero_index = jnp.zeros((), jnp.int32)
        key_index = head_index // group_size
        query_part = lax.dynamic_slice(query_rows, (seq_index, first_row, head_index, zero_index),
                                       (1, block_size, 1, head_dim)).reshape(block_size, head_dim)
        key_part = lax.dynamic_slice(key_rows, (seq_index, zero_index, key_index, zero_index),
                                     (1, seq_length, 1, head_dim)).reshape(seq_length, head_dim)
        value_part = lax.dynamic_slice(value_rows, (seq_index, zero_index, key_index, zero_index),
                                       (1, seq_length, 1, head_dim)).reshape(seq_length, head_dim)
        decay_row = lax.dynamic_slice(decay_sum, (seq_index, zero_index, head_index),
                                      (1, seq_length, 1)).reshape(seq_length)
        query_decay = lax.dynamic_slice_in_dim(decay_row, first_row, block_size)
        raw_scores = jnp.dot(query_part, key_part.T, preferred_element_type=jnp.float32)
        biased = raw_scores * score_scale + query_decay[:, None] - decay_row[None, :]
        allowed = positions[None, :] <= (first_row + offsets)[:, None]
        masked = jnp.where(allowed, biased, -jnp.inf)
        shifted = jnp.exp(masked - jnp.max(masked, axis=-1, keepdims=True))
        weights = (shifted / jnp.sum(shifted, axis=-1, keepdims=True)).astype(jnp.bfloat16)
        return jnp.dot(weights, value_part, preferred_element_type=jnp.float32).astype(jnp.bfloat16)

    flat_blocks = lax.map(one_block, jnp.arange(seq_count * head_count * block_count, dtype=jnp.int32))
    flat_blocks = flat_blocks.reshape(seq_count, head_count, block_count, block_size, head_dim)
    return flat_blocks.transpose(0, 2, 3, 1, 4).reshape(seq_count, seq_length, head_count * head_dim)
```

```python
import math

import jax
import jax.numpy as jnp
from jax import lax
from jax.experimental import pallas as pl
from jax.experimental.pallas import tpu as pltpu
from jax.sharding import PartitionSpec as P

MESH = pl.DeviceIdType.MESH
F32 = jnp.float32
BF16 = jnp.bfloat16
NT = (((1,), (1,)), ((), ()))
LOG2E = math.log2(math.e)


def flip(index, mask):
    bit = 1
    while bit <= mask:
        if mask & bit:
            index = index + bit * (1 - 2 * ((index // bit) % 2))
        bit *= 2
    return index


def last_bit(mask, half):
    if mask & 1:
        return 1
    return 1 << (mask.bit_length() - 1) if half == 0 else mask & -mask


def make_kernel(sp_count, dp_count, heads, key_heads, head_dim, rows, shard):
    half_shard = shard // 2
    local_heads = heads // 2
    local_keys = key_heads // 2
    group = heads // key_heads
    kw = local_keys * head_dim
    qw = local_heads * head_dim
    pairs = sp_count // 2
    span = 2 * rows
    bits = [1 << i for i in range(dp_count.bit_length() - 1)]
    masks = sorted(range(1, dp_count), key=lambda m: (bin(m).count("1"), m))
    score_scale = head_dim ** (-0.5) * LOG2E
    tile = 256

    def kernel(x_ref, wq_hbm, wk_hbm, wv_hbm, fw_ref, bias_ref, out_ref,
               xpeer, wkv, wq, qbuf, kvbuf, gbuf, gwide, drow, dcol, osend,
               local_sem, w_send, w_recv, x_sem, g_send, g_recv, kv_send, kv_recv,
               o_send, o_recv):
        s = lax.axis_index("sp")
        d = lax.axis_index("dp")
        parity = s % 2
        pair = s // 2
        peer = s + 1 - 2 * parity

        def own_rows(index):
            return pl.ds(pl.multiple_of(index * shard, shard), shard)

        locals_ = [
            pltpu.make_async_copy(
                wk_hbm.at[:, pl.ds(pl.multiple_of(parity * kw, kw), kw)],
                wkv.at[own_rows(d), pl.ds(0, kw)], local_sem.at[0]),
            pltpu.make_async_copy(
                wv_hbm.at[:, pl.ds(pl.multiple_of(parity * kw, kw), kw)],
                wkv.at[own_rows(d), pl.ds(kw, kw)], local_sem.at[1]),
            pltpu.make_async_copy(
                wq_hbm.at[:, pl.ds(pl.multiple_of(parity * qw, qw), qw)],
                wq.at[own_rows(d), :], local_sem.at[2]),
        ]
        for copy in locals_:
            copy.start()

        barrier = pltpu.get_barrier_semaphore()
        for k in range(1, sp_count):
            pl.semaphore_signal(barrier, inc=1, device_id={"sp": (s + k) % sp_count},
                                device_id_type=MESH)
        for b in bits:
            pl.semaphore_signal(barrier, inc=1, device_id={"dp": flip(d, b)},
                                device_id_type=MESH)
        pl.semaphore_wait(barrier, sp_count - 1 + len(bits))

        x_copy = pltpu.make_async_remote_copy(
            x_ref, xpeer, x_sem.at[0], x_sem.at[1], device_id={"sp": peer}, device_id_type=MESH)
        x_copy.start()

        buffers = (wkv, wq)

        def weight_copy(part, mask, half, bit):
            buffer = buffers[part]
            start = flip(d, mask) * shard + half * half_shard
            where = pl.ds(pl.multiple_of(start, half_shard), half_shard)
            there = mask | bit
            return pltpu.make_async_remote_copy(
                buffer.at[where, :], buffer.at[where, :],
                w_send.at[part, there, half], w_recv.at[part, there, half],
                device_id={"dp": flip(d, bit)}, device_id_type=MESH)

        sent = []

        def send(part, mask, half, bit):
            copy = weight_copy(part, mask, half, bit)
            copy.start()
            sent.append(copy)

        def arrive(part, mask, half):
            bit = last_bit(mask, half)
            start = flip(d, mask) * shard + half * half_shard
            where = pl.ds(pl.multiple_of(start, half_shard), half_shard)
            pltpu.make_async_remote_copy(
                buffers[part].at[where, :], buffers[part].at[where, :],
                w_send.at[part, mask, half], w_recv.at[part, mask, half],
                device_id={"dp": flip(d, bit)}, device_id_type=MESH).wait_recv()
            for b in reversed(bits):
                if not mask & b and last_bit(mask | b, half) == b:
                    send(part, mask, half, b)

        def first_half(bit):
            return 0 if bit == 2 else 1

        def direct(part, turn):
            for b in bits[1:] + bits[:1]:
                send(part, 0, (first_half(b) + turn) % 2, b)

        def order(items):
            return sorted(items, key=lambda mh: bin(mh[0]).count("1"))

        early = [(b, first_half(b)) for b in bits]
        late = [(b, 1 - first_half(b)) for b in bits]
        relayed = [(m, h) for m in masks if bin(m).count("1") > 1 for h in (0, 1)]

        locals_[0].wait()
        locals_[1].wait()
        direct(0, 0)
        direct(0, 1)
        locals_[2].wait()
        direct(1, 0)

        gate = lax.dot_general(fw_ref[...], x_ref[...], NT, preferred_element_type=F32)
        row_id = lax.broadcasted_iota(jnp.int32, (heads, 1), 0)
        bias = jnp.zeros((heads, 1), F32)
        for h in range(heads):
            bias = jnp.where(row_id == h, bias_ref[h], bias)
        gate = gate + bias
        log_gate = jnp.minimum(gate, 0.0) - jnp.log1p(jnp.exp(-jnp.abs(gate)))
        gbuf[s] = log_gate.astype(BF16)
        g_copies = []
        for k in range(1, sp_count):
            copy = pltpu.make_async_remote_copy(
                gbuf.at[s], gbuf.at[s], g_send.at[k], g_recv.at[s],
                device_id={"sp": (s + k) % sp_count}, device_id_type=MESH)
            copy.start()
            g_copies.append(copy)

        for m, h in early + late:
            arrive(0, m, h)
        direct(1, 1)
        for m, h in relayed:
            arrive(0, m, h)

        def project_kv(source, which):
            first = pl.multiple_of(which * rows, rows)

            def one(c, carry):
                cols = pl.ds(pl.multiple_of(c * tile, tile), tile)
                kvbuf[pair, pl.ds(first, rows), cols] = jnp.dot(
                    source[...], wkv[:, cols], preferred_element_type=F32).astype(BF16)
                return carry

            lax.fori_loop(0, 2 * kw // tile, one, 0)

        def kv_copy(source_pair, target_pair, which, part):
            where = pl.ds(pl.multiple_of(which * rows, rows), rows)
            return pltpu.make_async_remote_copy(
                kvbuf.at[source_pair, where], kvbuf.at[source_pair, where],
                kv_send.at[target_pair, part], kv_recv.at[source_pair, part],
                device_id={"sp": target_pair * 2 + parity}, device_id_type=MESH)

        def send_kv(which, part):
            for j in range(1, pairs):
                @pl.when(pair < j)
                def _():
                    kv_copy(pair, j, which, part).start()

        project_kv(x_ref, parity)
        send_kv(parity, 0)
        for m, h in early:
            arrive(1, m, h)

        x_copy.wait_recv()
        project_kv(xpeer, 1 - parity)
        send_kv(1 - parity, 1)

        for k in range(1, sp_count):
            source = (s + k) % sp_count
            pltpu.make_async_remote_copy(
                gbuf.at[source], gbuf.at[source], g_send.at[k], g_recv.at[source],
                device_id={"sp": source}, device_id_type=MESH).wait_recv()
        gwide[...] = gbuf[...].astype(F32)
        mine = pl.ds(pl.multiple_of(parity * local_heads, local_heads), local_heads)
        up_row = lax.broadcasted_iota(jnp.int32, (rows, span), 0)
        up_col = lax.broadcasted_iota(jnp.int32, (rows, span), 1)
        upper_a = jnp.where(up_row <= up_col, 1.0, 0.0).astype(BF16)
        upper_b = jnp.where(up_row + rows <= up_col, 1.0, 0.0).astype(BF16)
        low_row = lax.broadcasted_iota(jnp.int32, (span, rows), 0) + pair * span
        low_col = lax.broadcasted_iota(jnp.int32, (span, rows), 1)
        before = jnp.zeros((local_heads, 1), F32)
        column = jnp.zeros((span, local_heads), F32)
        for j in range(pairs):
            wide_a = gwide[2 * j, mine, :]
            wide_b = gwide[2 * j + 1, mine, :]
            gate_a = wide_a.astype(BF16)
            gate_b = wide_b.astype(BF16)
            inside = (jnp.dot(gate_a, upper_a, preferred_element_type=F32)
                      + jnp.dot(gate_b, upper_b, preferred_element_type=F32))
            drow[j] = (inside + before) * LOG2E
            before = (before + jnp.sum(wide_a, axis=1, keepdims=True)
                      + jnp.sum(wide_b, axis=1, keepdims=True))
            for block, gates in ((2 * j, gate_a), (2 * j + 1, gate_b)):
                lower = jnp.where(low_col + block * rows <= low_row, 1.0, 0.0).astype(BF16)
                column = column + lax.dot_general(lower, gates, NT, preferred_element_type=F32)
        dcol[...] = column * LOG2E

        for m, h in late + relayed:
            arrive(1, m, h)

        def project_q(c, carry):
            cols = pl.ds(pl.multiple_of(c * tile, tile), tile)
            own = pl.ds(pl.multiple_of(parity * rows, rows), rows)
            other = pl.ds(pl.multiple_of((1 - parity) * rows, rows), rows)
            qbuf[own, cols] = jnp.dot(
                x_ref[...], wq[:, cols], preferred_element_type=F32).astype(BF16)
            qbuf[other, cols] = jnp.dot(
                xpeer[...], wq[:, cols], preferred_element_type=F32).astype(BF16)
            return carry

        lax.fori_loop(0, qw // tile, project_q, 0)

        for j in range(pairs - 1):
            @pl.when(j < pair)
            def _():
                kv_copy(j, pair, parity, 0).wait_recv()
                kv_copy(j, pair, 1 - parity, 1).wait_recv()

        def out_copy(head):
            cols = pl.ds(pl.multiple_of(parity * qw + head * head_dim, head_dim), head_dim)
            return pltpu.make_async_remote_copy(
                osend.at[head], out_ref.at[:, cols], o_send.at[head], o_recv.at[head],
                device_id={"sp": peer}, device_id_type=MESH)

        def attend(turn, carry):
            block = (parity + 1 + turn) % 2
            where = pl.ds(pl.multiple_of(block * rows, rows), rows)
            row = lax.broadcasted_iota(jnp.int32, (rows, span), 0) + block * rows
            col = lax.broadcasted_iota(jnp.int32, (rows, span), 1)
            allowed = col <= row
            for head in range(local_heads):
                kh = head // group
                query = qbuf[where, head * head_dim:(head + 1) * head_dim]
                query_decay = dcol[where, head:head + 1]

                def scores(j):
                    key = kvbuf[j, :, kh * head_dim:(kh + 1) * head_dim]
                    raw = lax.dot_general(query, key, NT, preferred_element_type=F32)
                    return raw * score_scale + query_decay - drow[j, head:head + 1, :]

                def values(j):
                    return kvbuf[j, :, kw + kh * head_dim:kw + (kh + 1) * head_dim]

                sc = jnp.where(allowed, scores(pair), -jnp.inf)
                top = jnp.max(sc, axis=1, keepdims=True)
                weight = jnp.exp2(sc - top)
                total = jnp.sum(weight, axis=1, keepdims=True)
                acc = jnp.dot(weight.astype(BF16), values(pair), preferred_element_type=F32)

                def earlier(j, state):
                    top, total, acc = state
                    sc = scores(j)
                    new_top = jnp.maximum(top, jnp.max(sc, axis=1, keepdims=True))
                    keep = jnp.exp2(top - new_top)
                    weight = jnp.exp2(sc - new_top)
                    total = total * keep + jnp.sum(weight, axis=1, keepdims=True)
                    acc = acc * keep + jnp.dot(
                        weight.astype(BF16), values(j), preferred_element_type=F32)
                    return new_top, total, acc

                top, total, acc = lax.fori_loop(0, pair, earlier, (top, total, acc))
                result = (acc / total).astype(BF16)

                @pl.when(turn == 0)
                def _():
                    osend[head] = result
                    out_copy(head).start()

                @pl.when(turn == 1)
                def _():
                    cols = pl.ds(
                        pl.multiple_of(parity * qw + head * head_dim, head_dim), head_dim)
                    out_ref[:, cols] = result
            return carry

        lax.fori_loop(0, 2, attend, 0)

        x_copy.wait_send()
        for copy in sent + g_copies:
            copy.wait_send()
        for j in range(1, pairs):
            @pl.when(pair < j)
            def _():
                kv_copy(pair, j, parity, 0).wait_send()
                kv_copy(pair, j, 1 - parity, 1).wait_send()
        for head in range(local_heads):
            cols = pl.ds(pl.multiple_of((1 - parity) * qw + head * head_dim, head_dim), head_dim)
            out_copy(head).wait_send()
            pltpu.make_async_remote_copy(
                osend.at[head], out_ref.at[:, cols], o_send.at[head], o_recv.at[head],
                device_id={"sp": peer}, device_id_type=MESH).wait_recv()

    model = shard * dp_count
    scratch = [
        pltpu.VMEM((rows, model), BF16),
        pltpu.VMEM((model, 2 * kw), BF16),
        pltpu.VMEM((model, qw), BF16),
        pltpu.VMEM((span, qw), BF16),
        pltpu.VMEM((pairs, span, 2 * kw), BF16),
        pltpu.VMEM((sp_count, heads, rows), BF16),
        pltpu.VMEM((sp_count, heads, rows), F32),
        pltpu.VMEM((pairs, local_heads, span), F32),
        pltpu.VMEM((span, local_heads), F32),
        pltpu.VMEM((local_heads, rows, head_dim), BF16),
        pltpu.SemaphoreType.DMA((3,)),
        pltpu.SemaphoreType.DMA((2, dp_count, 2)),
        pltpu.SemaphoreType.DMA((2, dp_count, 2)),
        pltpu.SemaphoreType.DMA((2,)),
        pltpu.SemaphoreType.DMA((sp_count,)),
        pltpu.SemaphoreType.DMA((sp_count,)),
        pltpu.SemaphoreType.DMA((pairs, 2)),
        pltpu.SemaphoreType.DMA((pairs, 2)),
        pltpu.SemaphoreType.DMA((local_heads,)),
        pltpu.SemaphoreType.DMA((local_heads,)),
    ]
    return kernel, scratch


def solution(mesh):
    sp_count, dp_count = mesh.shape["sp"], mesh.shape["dp"]

    def on_device(tokens, query_weight, key_weight, value_weight, forget_weight, forget_bias):
        rows, model = tokens.shape[1:]
        heads = forget_weight.shape[1]
        head_dim = query_weight.shape[1] // heads
        key_heads = key_weight.shape[1] // head_dim
        kernel, scratch = make_kernel(
            sp_count, dp_count, heads, key_heads, head_dim, rows, query_weight.shape[0])
        vmem = pl.BlockSpec(memory_space=pltpu.VMEM)
        hbm = pl.BlockSpec(memory_space=pl.ANY)
        mixed = pl.pallas_call(
            kernel,
            out_shape=jax.ShapeDtypeStruct((rows, heads * head_dim), BF16),
            in_specs=[vmem, hbm, hbm, hbm, vmem, pl.BlockSpec(memory_space=pltpu.SMEM)],
            out_specs=vmem,
            scratch_shapes=scratch,
            compiler_params=pltpu.CompilerParams(
                collective_id=0, has_side_effects=True, vmem_limit_bytes=48 * 2**20),
            name="mixer",
        )(tokens[0], query_weight, key_weight, value_weight, forget_weight.T, forget_bias)
        return mixed[None]

    placed = (P("dp", "sp", None), P("dp", None), P("dp", None), P("dp", None), P(), P())
    return jax.shard_map(
        on_device, mesh=mesh, in_specs=placed, out_specs=P("dp", "sp", None), check_vma=False
    )
```

```python
import math

import jax
import jax.numpy as jnp
from jax import lax
from jax.experimental import pallas as pl
from jax.experimental.pallas import tpu as pltpu
from jax.sharding import PartitionSpec as P

MESH = pl.DeviceIdType.MESH
F32 = jnp.float32
BF16 = jnp.bfloat16
NT = (((1,), (1,)), ((), ()))
LOG2E = math.log2(math.e)


def flip(index, mask):
    bit = 1
    while bit <= mask:
        if mask & bit:
            index = index + bit * (1 - 2 * ((index // bit) % 2))
        bit *= 2
    return index


def last_bit(mask, half):
    if mask & 1:
        return 1
    return 1 << (mask.bit_length() - 1) if half == 0 else mask & -mask


def make_kernel(sp_count, dp_count, heads, key_heads, head_dim, rows, shard):
    half_shard = shard // 2
    local_heads = heads // 2
    local_keys = key_heads // 2
    group = heads // key_heads
    kw = local_keys * head_dim
    qw = local_heads * head_dim
    pairs = sp_count // 2
    span = 2 * rows
    bits = [1 << i for i in range(dp_count.bit_length() - 1)]
    masks = sorted(range(1, dp_count), key=lambda m: (bin(m).count("1"), m))
    score_scale = head_dim ** (-0.5) * LOG2E
    chunks = 4 if rows % 64 == 0 else 1
    chunk = rows // chunks
    kvw = 2 * head_dim
    ow = group * head_dim
    tile = 256

    def kernel(x_ref, wq_hbm, wk_hbm, wv_hbm, fw_ref, bias_ref, out_ref,
               xpeer, wkv, wq, qbuf, kvbuf, gbuf, gwide, drow, dcol, osend,
               local_sem, w_send, w_recv, x_send, x_recv, g_send, g_recv, kv_send, kv_recv,
               o_send, o_recv):
        s = lax.axis_index("sp")
        d = lax.axis_index("dp")
        parity = s % 2
        pair = s // 2
        peer = s + 1 - 2 * parity

        def own_rows(index):
            return pl.ds(pl.multiple_of(index * shard, shard), shard)

        def local_copy(source, first, width, target, index):
            return pltpu.make_async_copy(
                source.at[:, pl.ds(pl.multiple_of(first, width), width)], target,
                local_sem.at[index])

        locals_ = []
        for kh in range(local_keys):
            for i, source in enumerate((wk_hbm, wv_hbm)):
                locals_.append(local_copy(
                    source, parity * kw + kh * head_dim, head_dim,
                    wkv.at[own_rows(d), pl.ds(kh * kvw + i * head_dim, head_dim)],
                    kh * 3 + i))
        for kh in range(local_keys):
            locals_.append(local_copy(
                wq_hbm, parity * qw + kh * ow, ow, wq.at[kh, own_rows(d), :], kh * 3 + 2))
        for copy in locals_:
            copy.start()

        barrier = pltpu.get_barrier_semaphore()
        for k in range(1, sp_count):
            pl.semaphore_signal(barrier, inc=1, device_id={"sp": (s + k) % sp_count},
                                device_id_type=MESH)
        for b in bits:
            pl.semaphore_signal(barrier, inc=1, device_id={"dp": flip(d, b)},
                                device_id_type=MESH)
        pl.semaphore_wait(barrier, sp_count - 1 + len(bits))

        def x_copy(c):
            where = pl.ds(c * chunk, chunk)
            return pltpu.make_async_remote_copy(
                x_ref.at[where, :], xpeer.at[where, :], x_send.at[c], x_recv.at[c],
                device_id={"sp": peer}, device_id_type=MESH)

        for c in range(chunks):
            x_copy(c).start()

        def shard_ref(part, where):
            return wkv.at[where, :] if part == 0 else wq.at[part - 1, where, :]

        def weight_copy(part, mask, half, bit):
            start = flip(d, mask) * shard + half * half_shard
            where = pl.ds(pl.multiple_of(start, half_shard), half_shard)
            there = mask | bit
            return pltpu.make_async_remote_copy(
                shard_ref(part, where), shard_ref(part, where),
                w_send.at[part, there, half], w_recv.at[part, there, half],
                device_id={"dp": flip(d, bit)}, device_id_type=MESH)

        sent = []

        def send(part, mask, half, bit):
            copy = weight_copy(part, mask, half, bit)
            copy.start()
            sent.append(copy)

        def arrive(part, mask, half):
            bit = last_bit(mask, half)
            start = flip(d, mask) * shard + half * half_shard
            where = pl.ds(pl.multiple_of(start, half_shard), half_shard)
            pltpu.make_async_remote_copy(
                shard_ref(part, where), shard_ref(part, where),
                w_send.at[part, mask, half], w_recv.at[part, mask, half],
                device_id={"dp": flip(d, bit)}, device_id_type=MESH).wait_recv()
            for b in reversed(bits):
                if not mask & b and last_bit(mask | b, half) == b:
                    send(part, mask, half, b)

        def first_half(bit):
            return 0 if bit == 2 else 1

        def direct(part, turn):
            for b in bits[1:] + bits[:1]:
                send(part, 0, (first_half(b) + turn) % 2, b)

        early = [(b, first_half(b)) for b in bits]
        late = [(b, 1 - first_half(b)) for b in bits]
        relayed = [(m, h) for m in masks if bin(m).count("1") > 1 for h in (0, 1)]

        for copy in locals_[:2 * local_keys]:
            copy.wait()
        direct(0, 0)
        direct(0, 1)
        for copy in locals_[2 * local_keys:]:
            copy.wait()
        for m, h in early:
            arrive(0, m, h)
        direct(1, 0)
        direct(1, 1)

        gate = lax.dot_general(fw_ref[...], x_ref[...], NT, preferred_element_type=F32)
        row_id = lax.broadcasted_iota(jnp.int32, (heads, 1), 0)
        bias = jnp.zeros((heads, 1), F32)
        for h in range(heads):
            bias = jnp.where(row_id == h, bias_ref[h], bias)
        gate = gate + bias
        log_gate = jnp.minimum(gate, 0.0) - jnp.log1p(jnp.exp(-jnp.abs(gate)))
        gbuf[s] = log_gate.astype(BF16)
        g_copies = []
        for k in range(1, sp_count):
            copy = pltpu.make_async_remote_copy(
                gbuf.at[s], gbuf.at[s], g_send.at[k], g_recv.at[s],
                device_id={"sp": (s + k) % sp_count}, device_id_type=MESH)
            copy.start()
            g_copies.append(copy)

        for m, h in late + relayed:
            arrive(0, m, h)

        def kv_copy(source_pair, target_pair, which, kh, piece):
            if piece == 0:
                where = pl.ds(pl.multiple_of(which * rows, rows), rows)
            else:
                first = which * rows + (piece - 1) * chunk
                where = pl.ds(pl.multiple_of(first, chunk), chunk)
            return pltpu.make_async_remote_copy(
                kvbuf.at[source_pair, kh, where, :], kvbuf.at[source_pair, kh, where, :],
                kv_send.at[target_pair, kh, piece], kv_recv.at[source_pair, kh, piece],
                device_id={"sp": target_pair * 2 + parity}, device_id_type=MESH)

        def kv_pieces():
            return [(parity, 0)] + [(1 - parity, 1 + c) for c in range(chunks)]

        def project_kv(which, piece):
            if piece == 0:
                source, first, count = x_ref[...], which * rows, rows
            else:
                source = xpeer[(piece - 1) * chunk:piece * chunk, :]
                first, count = which * rows + (piece - 1) * chunk, chunk
            where = pl.ds(pl.multiple_of(first, count), count)
            for kh in range(local_keys):
                kvbuf[pair, kh, where, :] = jnp.dot(
                    source, wkv[:, kh * kvw:(kh + 1) * kvw],
                    preferred_element_type=F32).astype(BF16)
                for j in range(1, pairs):
                    @pl.when(pair < j)
                    def _():
                        kv_copy(pair, j, which, kh, piece).start()

        def peer_chunk(c):
            x_copy(c).wait_recv()
            project_kv(1 - parity, 1 + c)

        project_kv(parity, 0)
        for m, h in early:
            arrive(1, m, h)
        for part in range(2, 1 + local_keys):
            direct(part, 0)
            direct(part, 1)
        for c in range(chunks - 1):
            peer_chunk(c)

        for k in range(1, sp_count):
            source = (s + k) % sp_count
            pltpu.make_async_remote_copy(
                gbuf.at[source], gbuf.at[source], g_send.at[k], g_recv.at[source],
                device_id={"sp": source}, device_id_type=MESH).wait_recv()
        gwide[...] = gbuf[...].astype(F32)
        mine = pl.ds(pl.multiple_of(parity * local_heads, local_heads), local_heads)
        up_row = lax.broadcasted_iota(jnp.int32, (rows, span), 0)
        up_col = lax.broadcasted_iota(jnp.int32, (rows, span), 1)
        upper_a = jnp.where(up_row <= up_col, 1.0, 0.0).astype(BF16)
        upper_b = jnp.where(up_row + rows <= up_col, 1.0, 0.0).astype(BF16)
        low_row = lax.broadcasted_iota(jnp.int32, (span, rows), 0) + pair * span
        low_col = lax.broadcasted_iota(jnp.int32, (span, rows), 1)
        before = jnp.zeros((local_heads, 1), F32)
        column = jnp.zeros((span, local_heads), F32)
        for j in range(pairs):
            wide_a = gwide[2 * j, mine, :]
            wide_b = gwide[2 * j + 1, mine, :]
            gate_a = wide_a.astype(BF16)
            gate_b = wide_b.astype(BF16)
            inside = (jnp.dot(gate_a, upper_a, preferred_element_type=F32)
                      + jnp.dot(gate_b, upper_b, preferred_element_type=F32))
            sums = (inside + before) * LOG2E
            for kh in range(local_keys):
                drow[j, kh] = sums[kh * group:(kh + 1) * group]
            before = (before + jnp.sum(wide_a, axis=1, keepdims=True)
                      + jnp.sum(wide_b, axis=1, keepdims=True))
            for block, gates in ((2 * j, gate_a), (2 * j + 1, gate_b)):
                lower = jnp.where(low_col + block * rows <= low_row, 1.0, 0.0).astype(BF16)
                column = column + lax.dot_general(lower, gates, NT, preferred_element_type=F32)
        column = column * LOG2E
        for kh in range(local_keys):
            dcol[kh] = column[:, kh * group:(kh + 1) * group]

        peer_chunk(chunks - 1)

        def project_q(source, block, kh):
            where = pl.ds(pl.multiple_of(block * rows, rows), rows)

            def one(c, carry):
                cols = pl.ds(pl.multiple_of(c * tile, tile), tile)
                qbuf[kh, where, cols] = jnp.dot(
                    source[...], wq[kh, :, cols], preferred_element_type=F32).astype(BF16)
                return carry

            lax.fori_loop(0, ow // tile, one, 0)

        def out_copy(kh, half):
            cols = pl.ds(pl.multiple_of(half * qw + kh * ow, ow), ow)
            return pltpu.make_async_remote_copy(
                osend.at[kh], out_ref.at[:, cols], o_send.at[kh], o_recv.at[kh],
                device_id={"sp": peer}, device_id_type=MESH)

        def attend(block, kh, awaited):
            where = pl.ds(pl.multiple_of(block * rows, rows), rows)
            row = lax.broadcasted_iota(jnp.int32, (rows, span), 0) + block * rows
            col = lax.broadcasted_iota(jnp.int32, (rows, span), 1)
            allowed = col <= row

            def scores(j, g):
                query = qbuf[kh, where, g * head_dim:(g + 1) * head_dim]
                key = kvbuf[j, kh, :, :head_dim]
                raw = lax.dot_general(query, key, NT, preferred_element_type=F32)
                return raw * score_scale + dcol[kh, where, g:g + 1] - drow[j, kh, g:g + 1, :]

            def values(j):
                return kvbuf[j, kh, :, head_dim:]

            states = []
            for g in range(group):
                sc = jnp.where(allowed, scores(pair, g), -jnp.inf)
                top = jnp.max(sc, axis=1, keepdims=True)
                weight = jnp.exp2(sc - top)
                total = jnp.sum(weight, axis=1, keepdims=True)
                acc = jnp.dot(weight.astype(BF16), values(pair), preferred_element_type=F32)
                states.append((top, total, acc))

            def earlier(j, states):
                if awaited:
                    for which, piece in kv_pieces():
                        kv_copy(j, pair, which, kh, piece).wait_recv()
                after = []
                for g in range(group):
                    top, total, acc = states[g]
                    sc = scores(j, g)
                    new_top = jnp.maximum(top, jnp.max(sc, axis=1, keepdims=True))
                    keep = jnp.exp2(top - new_top)
                    weight = jnp.exp2(sc - new_top)
                    total = total * keep + jnp.sum(weight, axis=1, keepdims=True)
                    acc = acc * keep + jnp.dot(
                        weight.astype(BF16), values(j), preferred_element_type=F32)
                    after.append((new_top, total, acc))
                return tuple(after)

            states = lax.fori_loop(0, pair, earlier, tuple(states))
            return [(acc / total).astype(BF16) for _, total, acc in states]

        for m, h in late + relayed:
            arrive(1, m, h)
        for kh in range(local_keys):
            project_q(xpeer, 1 - parity, kh)
            for m, h in early if kh + 1 < local_keys else ():
                arrive(kh + 2, m, h)
            for g, result in enumerate(attend(1 - parity, kh, True)):
                osend[kh, :, g * head_dim:(g + 1) * head_dim] = result
            out_copy(kh, parity).start()
            for m, h in late + relayed if kh + 1 < local_keys else ():
                arrive(kh + 2, m, h)
        for kh in range(local_keys):
            project_q(x_ref, parity, kh)
            for g, result in enumerate(attend(parity, kh, False)):
                first = parity * qw + kh * ow + g * head_dim
                out_ref[:, pl.ds(pl.multiple_of(first, head_dim), head_dim)] = result

        for c in range(chunks):
            x_copy(c).wait_send()
        for copy in sent + g_copies:
            copy.wait_send()
        for j in range(1, pairs):
            @pl.when(pair < j)
            def _():
                for kh in range(local_keys):
                    for which, piece in kv_pieces():
                        kv_copy(pair, j, which, kh, piece).wait_send()
        for kh in range(local_keys):
            out_copy(kh, parity).wait_send()
            out_copy(kh, 1 - parity).wait_recv()

    model = shard * dp_count
    scratch = [
        pltpu.VMEM((rows, model), BF16),
        pltpu.VMEM((model, 2 * kw), BF16),
        pltpu.VMEM((local_keys, model, ow), BF16),
        pltpu.VMEM((local_keys, span, ow), BF16),
        pltpu.VMEM((pairs, local_keys, span, kvw), BF16),
        pltpu.VMEM((sp_count, heads, rows), BF16),
        pltpu.VMEM((sp_count, heads, rows), F32),
        pltpu.VMEM((pairs, local_keys, group, span), F32),
        pltpu.VMEM((local_keys, span, group), F32),
        pltpu.VMEM((local_keys, rows, group * head_dim), BF16),
        pltpu.SemaphoreType.DMA((3 * local_keys,)),
        pltpu.SemaphoreType.DMA((1 + local_keys, dp_count, 2)),
        pltpu.SemaphoreType.DMA((1 + local_keys, dp_count, 2)),
        pltpu.SemaphoreType.DMA((chunks,)),
        pltpu.SemaphoreType.DMA((chunks,)),
        pltpu.SemaphoreType.DMA((sp_count,)),
        pltpu.SemaphoreType.DMA((sp_count,)),
        pltpu.SemaphoreType.DMA((pairs, local_keys, 1 + chunks)),
        pltpu.SemaphoreType.DMA((pairs, local_keys, 1 + chunks)),
        pltpu.SemaphoreType.DMA((local_keys,)),
        pltpu.SemaphoreType.DMA((local_keys,)),
    ]
    return kernel, scratch


def solution(mesh):
    sp_count, dp_count = mesh.shape["sp"], mesh.shape["dp"]

    def on_device(tokens, query_weight, key_weight, value_weight, forget_weight, forget_bias):
        rows, model = tokens.shape[1:]
        heads = forget_weight.shape[1]
        head_dim = query_weight.shape[1] // heads
        key_heads = key_weight.shape[1] // head_dim
        kernel, scratch = make_kernel(
            sp_count, dp_count, heads, key_heads, head_dim, rows, query_weight.shape[0])
        vmem = pl.BlockSpec(memory_space=pltpu.VMEM)
        hbm = pl.BlockSpec(memory_space=pl.ANY)
        mixed = pl.pallas_call(
            kernel,
            out_shape=jax.ShapeDtypeStruct((rows, heads * head_dim), BF16),
            in_specs=[vmem, hbm, hbm, hbm, vmem, pl.BlockSpec(memory_space=pltpu.SMEM)],
            out_specs=vmem,
            scratch_shapes=scratch,
            compiler_params=pltpu.CompilerParams(
                collective_id=0, has_side_effects=True, vmem_limit_bytes=63 * 2**20),
            name="mixer",
        )(tokens[0], query_weight, key_weight, value_weight, forget_weight.T, forget_bias)
        return mixed[None]

    placed = (P("dp", "sp", None), P("dp", None), P("dp", None), P("dp", None), P(), P())
    return jax.shard_map(
        on_device, mesh=mesh, in_specs=placed, out_specs=P("dp", "sp", None), check_vma=False
    )
```
